32 devices in a mesh: sp: 8 (over z, y), tp: 4 (over x, core).
Axes of the slice: x: 2, y: 2, z: 4, core: 2. Of those that a mesh axis runs over, the one named last changes fastest.
Arguments:
- stream: bfloat16 [1536, 2048], P('sp'), may hold values from -6 to 6
- upstream: bfloat16 [1536, 2048], P('sp'), may hold values from -6 to 6
- expert_gain: float32 [2048], replicated, may hold values from 0.1 to 1.9
- expert_ids: int32 [1536, 2], P('sp'), may hold values from 0 to 7, all different within a row; in each aligned block of 192 rows (0 to 191, 192 to 383, ...) at most 60 rows name the same one
- group_weight: float32 [1536], P('sp'), may hold values from 0.25 to 1
- pair_scores: float32 [1536, 2], P('sp'), may hold values from -6 to 6
- gate_weight: bfloat16 [8, 2048, 1024], P('sp', None, 'tp'), may hold values from -0.125 to 0.125
- up_weight: bfloat16 [8, 2048, 1024], P('sp', None, 'tp'), may hold values from -0.125 to 0.125
- down_weight: bfloat16 [8, 1024, 2048], P('sp', 'tp'), may hold values from -0.1875 to 0.1875
- mixer_weight: bfloat16 [1024, 2048], P('tp'), may hold values from -0.1875 to 0.1875
- filtered: bfloat16 [1536, 1024], P('sp', 'tp'), may hold values from -1000 to 1000
- channel_gain: float32 [1024], P('tp'), may hold values from 0.1 to 1.9
- kernel_taps: float32 [31, 1024], P(None, 'tp'), may hold values from -1 to 1
- value_branch: bfloat16 [1536, 1024], P('sp', 'tp'), may hold values from -6 to 6
- gate_branch: bfloat16 [1536, 1024], P('sp', 'tp'), may hold values from -6 to 6
Outputs:
- gradient_value: bfloat16 [1536, 1024], P('sp', 'tp')
- gradient_gating: bfloat16 [1536, 1024], P('sp', 'tp')
- gradient_mixer: float32 [2048, 1024], P('sp', 'tp')
- gradient_gate: float32 [8, 2048, 1024], P('sp', None, 'tp')
- gradient_up: float32 [8, 2048, 1024], P('sp', None, 'tp')
- gradient_down: float32 [8, 1024, 2048], P('sp', 'tp')
The draws below stay inside these ranges and needn't reach their ends.
Inputs may be any that keep to these rules, and one draw needn't show every extreme that they name: `expert_ids`: the two experts of a token differ. Among the rows of one index of sp, at most 60 routes name the same expert, and in every draw some expert is named by exactly 60 of them.
All inputs are finite; a program needn't handle non-finite values.
Results may differ from the reference program's by a relative error of at most 0.012.
Values may be sent and summed in bfloat16 or wider, within the bound.
No kernel may reach another device: no remote copies, remote signals or barrier semaphores. Data moves between devices by JAX's collectives and lax.ppermute only.
A program may use at most 64 MiB of HBM per device.

```python
import math
import jax
import jax.numpy as jnp
import numpy as np
from jax import lax

D = 2048
C = 1024
F = 1024
K = 31
TOK_DEV = 192
TOKENS = 1536
EXPERTS = 8
CAP = 60
N_SP = 8
N_TP = 4


def draw_filtered(key, part):
    keys = jax.random.split(jax.random.fold_in(key, 17), 3)
    jitter = jax.random.uniform(keys[0], (C,), jnp.float32, 0.0, 1.0)
    channel_scale = jnp.exp(jnp.log(10.0) * (jnp.arange(C, dtype=jnp.float32) + jitter * C / 4.0) / (1.25 * C))
    row_scale = jnp.exp(jax.random.uniform(keys[1], (TOKENS, 1), jnp.float32, 0.0, jnp.log(10.0)))
    values = jax.random.normal(keys[2], (TOKENS, C), jnp.float32) * channel_scale * row_scale
    return jnp.clip(values, -1000.0, 1000.0).astype(jnp.bfloat16)


def strengthened(array, stream_key, source, target, parts, factor):
    owner, partner = [(jnp.arange(array.shape[dim]) // (array.shape[dim] // parts)).reshape([-1 if axis == dim else 1 for axis in range(array.ndim)]) for dim in (source, target)]
    chosen = jax.random.permutation(stream_key, parts)[partner]
    strong = (owner == chosen) | (owner == (partner + parts // 2) % parts)
    return jnp.where(strong, factor * array, array)


def level_of(key, shape, cuts, low, top_value):
    gain, own = 1.0, jax.random.fold_in(key, 6)
    for axis_at, blocks in cuts:
        draws = jnp.exp(jax.random.uniform(jax.random.fold_in(own, axis_at), (blocks,), jnp.float32, low / len(cuts), top_value / len(cuts)))
        gain = gain * jnp.repeat(draws, shape[axis_at] // blocks).reshape([-1 if axis == axis_at else 1 for axis in range(len(shape))])
    return gain


def shared_out(own_key, own, number, rows, number_of, top, limit, slope):
    ranking = jax.random.permutation(own_key, number_of)
    heavy_load, ordinary = load_shares(number_of, rows * top, limit, slope, True), load_shares(number_of, rows * top, limit, slope, False)
    places = jnp.arange(number_of)

    def named(sizes, offset_by):
        used = int((sizes > 0).sum())
        fixed = max(1, used // 4)
        shifted = fixed + (places - fixed + offset_by * (used - fixed)) % max(1, number_of - fixed)
        return jnp.zeros((number_of,), jnp.int32).at[ranking[jnp.where(places < fixed, places, shifted)]].set(jnp.asarray(sizes, jnp.int32))

    sizes = jnp.where(number % 4 == 0, named(heavy_load, number // 4), named(ordinary, number - number // 4 - 1))
    mixed = jax.random.permutation(jax.random.fold_in(own, 3), number_of)
    giver, sink = mixed[0:number_of // 2 * 2:2], mixed[1:number_of // 2 * 2:2]
    room = jnp.minimum(sizes[giver] - 1, limit - sizes[sink]) // 2
    room = jnp.where((giver == ranking[0]) | (sink == ranking[0]) | (sizes[sink] == 0), 0, jnp.maximum(room, 0))
    shifted = jax.random.randint(jax.random.fold_in(own, 4), (number_of // 2,), 0, 1 << 20) % (room + 1)
    sizes = sizes.at[giver].add(-shifted).at[sink].add(shifted)
    items = jnp.searchsorted(jnp.cumsum(sizes), jnp.arange(rows * top), side="right").astype(jnp.int32)
    listing = items.reshape(top, rows).T
    listing = listing[jax.random.permutation(jax.random.fold_in(own, 1), rows)]
    offset_by = jax.random.randint(jax.random.fold_in(own, 2), (rows, 1), 0, top)
    return jnp.take_along_axis(listing, (jnp.arange(top)[None, :] + offset_by) % top, axis=1)


def load_shares(amount, total, reach, skew, full):
    weights = [(1 << 20) // math.isqrt(grade ** skew) + 1 for grade in range(1, amount + 1)]
    largest = reach if full else min(reach, max(-(-total // amount), total * weights[0] // sum(weights)))
    least = 1 if total - largest >= amount - 1 else 0
    holding, spare = [largest] + [least] * (amount - 1), total - largest - least * (amount - 1)
    while spare > 0:
        free = [i for i in range(1, amount) if holding[i] < largest] or [i for i in range(1, amount) if holding[i] < reach]
        mass, left = sum([weights[i] for i in free]), spare
        for i in free:
            addition = min(reach - holding[i], max(1, left * weights[i] // mass), spare)
            holding[i] = holding[i] + addition
            spare = spare - addition
    return np.array(holding)


def noise(rng, shape, width, limit, cuts=(), held_as=jnp.bfloat16):
    values = width * jax.random.normal(rng, shape, jnp.float32)
    if cuts:
        values = values * level_of(rng, shape, cuts, -0.22, 0.18)
    return jnp.clip(values, -limit, limit).astype(held_as)


def gaussian_with(stream_key, shape, deviation, bound, shards, heavy, kind=jnp.bfloat16):
    array = deviation * jax.random.normal(stream_key, shape, jnp.float32)
    if shards:
        array = array * level_of(stream_key, shape, shards, -0.22, 0.18)
    return jnp.clip(strengthened(array, jax.random.fold_in(stream_key, 3), *heavy), -bound, bound).astype(kind)


def setup_inputs(seed: int = 0) -> dict:
    key_of = jax.random.split(jax.random.key(seed), 16)
    stream = noise(key_of[0], (TOKENS, D), 1.0, 6.0, ((0, 8),))
    upstream = gaussian_with(key_of[1], (TOKENS, D), 1.0, 6.0, ((0, 8),), (0, 1, 8, 2.0))
    expert_gain = jnp.clip(1.0 + 0.18 * jax.random.normal(key_of[2], (D,), jnp.float32), 0.1, 1.9)
    expert_ids_keys = jax.random.split(jax.random.fold_in(key_of[3], 1), TOKENS // TOK_DEV)
    expert_ids_turns = jax.random.permutation(jax.random.fold_in(key_of[3], 3), TOKENS // TOK_DEV)
    expert_ids = jax.vmap(lambda own, number: shared_out(jax.random.fold_in(key_of[3], 2), own, number, TOK_DEV, EXPERTS, 2, CAP, 1))(expert_ids_keys, expert_ids_turns).reshape((TOKENS, 2))
    group_weight = jnp.clip(0.25 + 0.75 * jax.random.uniform(key_of[4], (TOKENS,), jnp.float32) ** level_of(key_of[4], (TOKENS,), ((0, 8),), -0.2, 0.2), 0.25, 1.0)
    pair_scores = noise(key_of[5], (TOKENS, 2), 1.5, 6.0, ((0, 8),), jnp.float32)
    gate_weight = noise(key_of[6], (EXPERTS, D, F), D ** -0.5, 0.125, ((0, 8), (2, 4)))
    up_weight = noise(key_of[7], (EXPERTS, D, F), D ** -0.5, 0.125, ((0, 8), (2, 4)))
    down_weight = noise(key_of[8], (EXPERTS, F, D), F ** -0.5, 0.1875, ((0, 8), (1, 4)))
    mixer_weight = noise(key_of[9], (C, D), C ** -0.5, 0.1875, ((0, 4),))
    filtered = draw_filtered(jax.random.fold_in(key_of[15], 71), 0)
    channel_gain = jnp.clip(1.0 + 0.18 * jax.random.normal(key_of[11], (C,), jnp.float32), 0.1, 1.9)
    kernel_taps = noise(key_of[12], (K, C), K ** -0.5, 1.0, ((1, 4),), jnp.float32)
    value_branch = noise(key_of[13], (TOKENS, C), 1.0, 6.0, ((0, 8), (1, 4)))
    gate_branch = noise(key_of[14], (TOKENS, C), 1.5, 6.0, ((0, 8), (1, 4)))
    return dict(stream=stream, upstream=upstream, expert_gain=expert_gain, expert_ids=expert_ids, group_weight=group_weight, pair_scores=pair_scores, gate_weight=gate_weight, up_weight=up_weight, down_weight=down_weight, mixer_weight=mixer_weight, filtered=filtered, channel_gain=channel_gain, kernel_taps=kernel_taps, value_branch=value_branch, gate_branch=gate_branch)


EPS = 1e-06

def route_slots(routes, capacity, experts):
    flat = routes.reshape(-1)
    onehot = (flat[:, None] == jnp.arange(experts, dtype=jnp.int32)[None, :]).astype(jnp.int32)
    before = jnp.cumsum(onehot, axis=0) - onehot
    position = lax.optimization_barrier(jnp.sum(before * onehot, axis=1))
    slots = (flat * capacity + position).astype(jnp.int32)
    total = flat.shape[0]
    source = jnp.full((experts * capacity,), total, jnp.int32).at[slots].set(jnp.arange(total, dtype=jnp.int32))
    return (slots, source)

def silu_slope(value, sigma):
    return sigma * (1.0 + value * (1.0 - sigma))

def reference(stream, upstream, expert_gain, expert_ids, group_weight, pair_scores, gate_weight, up_weight, down_weight, mixer_weight, filtered, channel_gain, kernel_taps, value_branch, gate_branch):
    stream_f = stream.astype(jnp.float32)
    inv_rms = lax.rsqrt(lax.optimization_barrier(jnp.mean(stream_f * stream_f, axis=1, keepdims=True)) + EPS)
    normed = (stream_f * inv_rms * expert_gain).astype(jnp.bfloat16)
    spread = pair_scores[:, 0] - pair_scores[:, 1]
    route_weight = group_weight[:, None] * jnp.stack([jax.nn.sigmoid(spread), jax.nn.sigmoid(-spread)], axis=1)
    per_block = expert_ids.reshape(N_SP, TOK_DEV, 2)
    slots, source = jax.vmap(lambda routes: route_slots(routes, CAP, EXPERTS))(per_block)
    routes_dev = 2 * TOK_DEV
    offsets = (jnp.arange(N_SP, dtype=jnp.int32) * routes_dev)[:, None]
    global_source = jnp.where(source < routes_dev, source + offsets, 2 * TOKENS).astype(jnp.int32)
    table = global_source.reshape(N_SP, EXPERTS, CAP).transpose(1, 0, 2).reshape(EXPERTS, N_SP * CAP)
    normed_ext = jnp.concatenate([normed, jnp.zeros((1, D), jnp.bfloat16)], axis=0)
    upstream_ext = jnp.concatenate([upstream, jnp.zeros((1, D), jnp.bfloat16)], axis=0)
    weight_ext = jnp.concatenate([route_weight.reshape(-1), jnp.zeros((1,), jnp.float32)], axis=0)
    block = F // N_TP

    def one_expert(args):
        index, gate_w, up_w, down_w = args
        token_index = index // 2
        rows = normed_ext[token_index]
        cots = (weight_ext[index][:, None] * upstream_ext[token_index].astype(jnp.float32)).astype(jnp.bfloat16)
        pre_gate = jnp.dot(rows, gate_w, preferred_element_type=jnp.float32)
        pre_up = jnp.dot(rows, up_w, preferred_element_type=jnp.float32)
        sigma = jax.nn.sigmoid(pre_gate)
        silu_gate = pre_gate * sigma
        hidden = (silu_gate * pre_up).astype(jnp.bfloat16)
        grad_hidden = jnp.dot(cots, down_w.T, preferred_element_type=jnp.float32)
        grad_pre_gate = (grad_hidden * pre_up * silu_slope(pre_gate, sigma)).astype(jnp.bfloat16)
        grad_pre_up = (grad_hidden * silu_gate).astype(jnp.bfloat16)
        grad_gate_w = jnp.dot(rows.T, grad_pre_gate, preferred_element_type=jnp.float32)
        grad_up_w = jnp.dot(rows.T, grad_pre_up, preferred_element_type=jnp.float32)
        grad_down_w = jnp.dot(hidden.T, cots, preferred_element_type=jnp.float32)
        terms = jnp.einsum('rtf,dtf->trd', grad_pre_gate.reshape(-1, N_TP, block).astype(jnp.float32), gate_w.reshape(D, N_TP, block).astype(jnp.float32))
        terms = terms + jnp.einsum('rtf,dtf->trd', grad_pre_up.reshape(-1, N_TP, block).astype(jnp.float32), up_w.reshape(D, N_TP, block).astype(jnp.float32))
        rounded = lax.optimization_barrier(terms.astype(jnp.bfloat16))
        returned = lax.optimization_barrier(jnp.sum(rounded.astype(jnp.float32), axis=0)).astype(jnp.bfloat16)
        return (grad_gate_w, grad_up_w, grad_down_w, returned)
    gradient_gate, gradient_up, gradient_down, returned = lax.map(one_expert, (table, gate_weight, up_weight, down_weight))
    returned_flat = returned.reshape(EXPERTS * N_SP * CAP, D)
    expert_of = slots // CAP
    position = slots % CAP
    flat_index = (expert_of * (N_SP * CAP) + jnp.arange(N_SP, dtype=jnp.int32)[:, None] * CAP + position).astype(jnp.int32).reshape(TOKENS, 2)
    grad_normed = returned_flat[flat_index[:, 0]].astype(jnp.float32) + returned_flat[flat_index[:, 1]].astype(jnp.float32)
    weighted = grad_normed * expert_gain
    inner = lax.optimization_barrier(jnp.mean(weighted * stream_f, axis=1, keepdims=True))
    grad_stream = (upstream.astype(jnp.float32) + inv_rms * weighted - stream_f * inv_rms * inv_rms * inv_rms * inner).astype(jnp.bfloat16)
    grad_act = jnp.dot(grad_stream, mixer_weight.T, preferred_element_type=jnp.float32)
    filt = filtered.astype(jnp.float32)
    mean_c = lax.optimization_barrier(jnp.mean(filt, axis=1, keepdims=True))
    raw = filt - mean_c
    inv_std = lax.rsqrt(lax.optimization_barrier(jnp.mean(raw * raw, axis=1, keepdims=True)) + EPS)
    centred = raw * inv_std
    normal_out = centred * channel_gain
    sigma = jax.nn.sigmoid(normal_out)
    activated = (normal_out * sigma).astype(jnp.bfloat16)
    gradient_mixer = jnp.dot(grad_stream.T, activated, preferred_element_type=jnp.float32)
    grad_centred = grad_act * silu_slope(normal_out, sigma) * channel_gain
    first_mean = lax.optimization_barrier(jnp.mean(grad_centred, axis=1, keepdims=True))
    second_mean = lax.optimization_barrier(jnp.mean(grad_centred * centred, axis=1, keepdims=True))
    grad_filtered = (inv_std * (grad_centred - first_mean - centred * second_mean)).astype(jnp.bfloat16)
    extended = jnp.concatenate([grad_filtered.astype(jnp.float32), jnp.zeros((K - 1, C), jnp.float32)], axis=0)
    grad_mixed = lax.conv_general_dilated(extended[None], kernel_taps[::-1][:, None, :], (1,), 'VALID', dimension_numbers=('NWC', 'WIO', 'NWC'), feature_group_count=C, precision=lax.Precision.HIGHEST)[0]
    sig_gate = jax.nn.sigmoid(gate_branch.astype(jnp.float32))
    gradient_value = (grad_mixed * sig_gate).astype(jnp.bfloat16)
    gradient_gating = (grad_mixed * value_branch.astype(jnp.float32) * sig_gate * (1.0 - sig_gate)).astype(jnp.bfloat16)
    return (gradient_value, gradient_gating, gradient_mixer, gradient_gate, gradient_up, gradient_down)
```

```python
import jax
import jax.numpy as jnp
from jax import lax
from jax.sharding import PartitionSpec as P

EPS = 1e-06


def swap(block, axis, mask):
    return lax.ppermute(block, axis, [(i, i ^ mask) for i in range(lax.axis_size(axis))])


def small(axis):
    size = lax.axis_size(axis)
    return size <= 8 and size & (size - 1) == 0


def exchange(blocks, axis):
    if small(axis):
        return [blocks[0]] + [swap(blocks[s], axis, s) for s in range(1, len(blocks))]
    moved = lax.all_to_all(jnp.stack(blocks), axis, split_axis=0, concat_axis=0, tiled=True)
    return [moved[s] for s in range(len(blocks))]


def gather_tokens(block, axis):
    size = lax.axis_size(axis)
    if not small(axis):
        return lax.all_gather(block, axis, axis=0, tiled=True)
    if size < 4:
        return jnp.concatenate([block] + [swap(block, axis, s) for s in range(1, size)], axis=0)
    even = jnp.stack([block] + [swap(block, axis, s) for s in range(2, size, 2)])
    odd = swap(even, axis, 1)
    rows, cols = block.shape
    return jnp.stack([even, odd], axis=1).reshape(size * rows, cols)


def gather_columns(block, axis):
    if lax.axis_size(axis) != 4:
        return lax.all_gather(block, axis, axis=1, tiled=True)
    index = lax.axis_index(axis)
    far, near = index // 2 == 0, index % 2 == 0
    other = swap(block, axis, 2)
    width = block.shape[1]
    pair = jnp.concatenate([jnp.where(far, block, other), jnp.where(far, other, block)], axis=1)
    over = swap(pair, axis, 1)
    first, second = jnp.where(near, pair, over), jnp.where(near, over, pair)
    return jnp.concatenate(
        [first[:, :width], second[:, :width], first[:, width:], second[:, width:]], axis=1
    )


def scatter_columns(partial, axis):
    if lax.axis_size(axis) != 4:
        return lax.psum_scatter(
            partial.astype(jnp.bfloat16), axis, scatter_dimension=1, tiled=True
        )
    index = lax.axis_index(axis)
    far, near = index // 2 == 0, index % 2 == 0
    a, b, c, d = jnp.split(partial, 4, axis=1)
    give = jnp.concatenate([jnp.where(near, b, a), jnp.where(near, d, c)], axis=1)
    keep = jnp.concatenate([jnp.where(near, a, b), jnp.where(near, c, d)], axis=1)
    keep = keep + swap(give.astype(jnp.bfloat16), axis, 1).astype(jnp.float32)
    low, high = jnp.split(keep, 2, axis=1)
    give = jnp.where(far, high, low).astype(jnp.bfloat16)
    own = jnp.where(far, low, high)
    return (own + swap(give, axis, 2).astype(jnp.float32)).astype(jnp.bfloat16)


def gather_small(value, axis):
    if small(axis):
        return [value] + [swap(value, axis, s) for s in range(1, lax.axis_size(axis))]
    moved = lax.all_gather(value, axis, axis=0)
    return [moved[s] for s in range(lax.axis_size(axis))]


def shifted(block, axis, distance):
    devices = range(lax.axis_size(axis))
    route = [(i - distance, i) for i in devices if i - distance in devices]
    return lax.ppermute(block, axis, route)


def silu_slope(value, sigma):
    return sigma * (1.0 + value * (1.0 - sigma))


def contract_last(left, right):
    return lax.dot_general(
        left, right, (((1,), (1,)), ((), ())), preferred_element_type=jnp.float32
    )


def contract_first(left, right):
    return lax.dot_general(
        left, right, (((0,), (0,)), ((), ())), preferred_element_type=jnp.float32
    )


def body(
    stream,
    upstream,
    expert_gain,
    expert_ids,
    group_weight,
    pair_scores,
    gate_weight,
    up_weight,
    down_weight,
    mixer_weight,
    filtered,
    channel_gain,
    kernel_taps,
    value_branch,
    gate_branch,
):
    experts = lax.axis_size("sp")
    tokens_here, width = stream.shape
    capacity = max(2, 5 * tokens_here // (2 * experts))
    room = -(-capacity // 8) * 8
    groups = lax.axis_size("tp")
    column = width // groups
    first_col = lax.axis_index("tp") * column
    bf16 = jnp.bfloat16

    ids = expert_ids.T
    block_of = ids ^ lax.axis_index("sp") if small("sp") else ids
    lanes = jnp.arange(experts, dtype=jnp.int32)
    named = [(block_of[k][None, :] == lanes[:, None]).astype(jnp.float32) for k in (0, 1)]
    both = (named[0] + named[1]).astype(bf16)
    order = jnp.arange(tokens_here, dtype=jnp.int32)
    earlier = (order[:, None] < order[None, :]).astype(bf16)
    before = jnp.dot(both, earlier, preferred_element_type=jnp.float32)
    slots = [
        block_of[k] * room + jnp.sum(before * named[k], axis=0).astype(jnp.int32) for k in (0, 1)
    ]
    places = jnp.arange(experts * room, dtype=jnp.int32)
    hit0 = places[:, None] == slots[0][None, :]
    hit1 = places[:, None] == slots[1][None, :]
    pick = (hit0 | hit1).astype(bf16)
    spread = pair_scores[:, 0] - pair_scores[:, 1]
    weight0 = group_weight * jax.nn.sigmoid(spread)
    weight1 = group_weight * jax.nn.sigmoid(-spread)
    slot_weight = jnp.sum(
        jnp.where(hit0, weight0[None, :], 0.0) + jnp.where(hit1, weight1[None, :], 0.0), axis=1
    )

    stream_f = stream.astype(jnp.float32)
    inv_rms = lax.rsqrt(jnp.mean(stream_f * stream_f, axis=1, keepdims=True) + EPS)
    stream_part = lax.dynamic_slice_in_dim(stream, first_col, column, 1).astype(jnp.float32)
    gain_part = lax.dynamic_slice_in_dim(expert_gain, first_col, column, 0)
    upstream_part = lax.dynamic_slice_in_dim(upstream, first_col, column, 1)
    normed_part = (stream_part * inv_rms * gain_part).astype(bf16)
    send_rows = jnp.dot(pick, normed_part, preferred_element_type=jnp.float32).astype(bf16)
    send_cots = (
        slot_weight[:, None] * jnp.dot(pick, upstream_part, preferred_element_type=jnp.float32)
    ).astype(bf16)

    def block_list(array):
        return [array[s * room : (s + 1) * room] for s in range(experts)]

    got_rows = jnp.concatenate(exchange(block_list(send_rows), "sp"), axis=0)
    got_cots = jnp.concatenate(exchange(block_list(send_cots), "sp"), axis=0)
    rows = gather_columns(got_rows, "tp")
    cots = gather_columns(got_cots, "tp")

    filt = filtered.astype(jnp.float32)
    here = filt.shape[1]
    channels = here * groups
    own_mean = jnp.mean(filt, axis=1)
    own_square = jnp.sum((filt - own_mean[:, None]) ** 2, axis=1)
    stats = gather_small(jnp.stack([own_mean, own_square]), "tp")
    mean_c = sum(part[0] for part in stats) / groups
    squares = sum(part[1] + here * (part[0] - mean_c) ** 2 for part in stats)
    inv_std = lax.rsqrt(squares / channels + EPS)[:, None]
    centred = (filt - mean_c[:, None]) * inv_std
    normal_out = centred * channel_gain
    sig_norm = jax.nn.sigmoid(normal_out)
    activated = (normal_out * sig_norm).astype(bf16)
    slope = silu_slope(normal_out, sig_norm) * channel_gain

    gate_local = gate_weight[0]
    up_local = up_weight[0]
    down_local = down_weight[0]
    pre_gate = jnp.dot(rows, gate_local, preferred_element_type=jnp.float32)
    pre_up = jnp.dot(rows, up_local, preferred_element_type=jnp.float32)
    sigma = jax.nn.sigmoid(pre_gate)
    silu_gate = pre_gate * sigma
    hidden = (silu_gate * pre_up).astype(bf16)
    grad_hidden = contract_last(cots, down_local)
    grad_pre_gate = (grad_hidden * pre_up * silu_slope(pre_gate, sigma)).astype(bf16)
    grad_pre_up = (grad_hidden * silu_gate).astype(bf16)
    partial_rows = contract_last(grad_pre_gate, gate_local) + contract_last(grad_pre_up, up_local)
    shared = scatter_columns(partial_rows, "tp")
    back = jnp.concatenate(exchange(block_list(shared), "sp"), axis=0)
    activated, shared = lax.optimization_barrier((activated, shared))
    all_activated = gather_tokens(activated, "sp")
    gradient_gate = contract_first(rows, grad_pre_gate)[None]
    gradient_up = contract_first(rows, grad_pre_up)[None]
    gradient_down = contract_first(hidden, cots)[None]

    grad_part = contract_first(pick, back).astype(bf16)
    grad_normed = gather_columns(grad_part, "tp").astype(jnp.float32)
    weighted = grad_normed * expert_gain
    inner = jnp.mean(weighted * stream_f, axis=1, keepdims=True)
    grad_stream = (
        upstream.astype(jnp.float32)
        + inv_rms * weighted
        - stream_f * inv_rms * inv_rms * inv_rms * inner
    ).astype(bf16)
    share = width // experts
    sent = [grad_stream[:, s * share : (s + 1) * share] for s in range(experts)]
    if small("sp"):
        me = lax.axis_index("sp")
        sent = [
            lax.dynamic_slice_in_dim(grad_stream, (me ^ s) * share, share, 1)
            for s in range(experts)
        ]
    all_grads = jnp.concatenate(exchange(sent, "sp"), axis=0)
    gradient_mixer = contract_first(all_grads, all_activated)

    grad_act = contract_last(grad_stream, mixer_weight)
    grad_centred = grad_act * slope
    sums = gather_small(
        jnp.stack([jnp.sum(grad_centred, axis=1), jnp.sum(grad_centred * centred, axis=1)]), "tp"
    )
    slope_sum, slope_cross = sum(sums[1:], sums[0]) / channels
    grad_filtered = (
        inv_std * (grad_centred - slope_sum[:, None] - centred * slope_cross[:, None])
    ).astype(bf16)
    reach = kernel_taps.shape[0] - 1
    ahead = shifted(grad_filtered[:reach], "sp", -1)
    extended = jnp.concatenate([grad_filtered, ahead], axis=0).astype(jnp.float32)
    grad_mixed = lax.conv_general_dilated(
        extended[None],
        kernel_taps[::-1][:, None, :],
        (1,),
        "VALID",
        dimension_numbers=("NWC", "WIO", "NWC"),
        feature_group_count=here,
        precision=lax.Precision.HIGHEST,
    )[0]
    sig_gate = jax.nn.sigmoid(gate_branch.astype(jnp.float32))
    gradient_value = (grad_mixed * sig_gate).astype(bf16)
    gradient_gating = (
        grad_mixed * value_branch.astype(jnp.float32) * sig_gate * (1.0 - sig_gate)
    ).astype(bf16)
    return (
        gradient_value,
        gradient_gating,
        gradient_mixer,
        gradient_gate,
        gradient_up,
        gradient_down,
    )


def solution(mesh):
    return jax.shard_map(
        body,
        mesh=mesh,
        in_specs=(
            P("sp", None),
            P("sp", None),
            P(),
            P("sp", None),
            P("sp"),
            P("sp", None),
            P("sp", None, "tp"),
            P("sp", None, "tp"),
            P("sp", "tp", None),
            P("tp", None),
            P("sp", "tp"),
            P("tp"),
            P(None, "tp"),
            P("sp", "tp"),
            P("sp", "tp"),
        ),
        out_specs=(
            P("sp", "tp"),
            P("sp", "tp"),
            P("sp", "tp"),
            P("sp", None, "tp"),
            P("sp", None, "tp"),
            P("sp", "tp", None),
        ),
        check_vma=False,
    )
```

```python
import jax
import jax.numpy as jnp
from jax import lax
from jax.sharding import PartitionSpec as P

EPS = 1e-06


def swap(block, axis, mask):
    return lax.ppermute(block, axis, [(i, i ^ mask) for i in range(lax.axis_size(axis))])


def small(axis):
    size = lax.axis_size(axis)
    return size <= 8 and size & (size - 1) == 0


def exchange(blocks, axis):
    if small(axis):
        return [blocks[0]] + [swap(blocks[s], axis, s) for s in range(1, len(blocks))]
    moved = lax.all_to_all(jnp.stack(blocks), axis, split_axis=0, concat_axis=0, tiled=True)
    return [moved[s] for s in range(len(blocks))]


def gather_tokens(block, axis):
    size = lax.axis_size(axis)
    if not small(axis):
        return lax.all_gather(block, axis, axis=0, tiled=True)
    if size < 4:
        return jnp.concatenate([block] + [swap(block, axis, s) for s in range(1, size)], axis=0)
    even = jnp.stack([block] + [swap(block, axis, s) for s in range(2, size, 2)])
    odd = swap(even, axis, 1)
    rows, cols = block.shape
    return jnp.stack([even, odd], axis=1).reshape(size * rows, cols)


def gather_columns(block, axis):
    if lax.axis_size(axis) != 4:
        return lax.all_gather(block, axis, axis=1, tiled=True)
    index = lax.axis_index(axis)
    far, near = index // 2 == 0, index % 2 == 0
    other = swap(block, axis, 2)
    width = block.shape[1]
    pair = jnp.concatenate([jnp.where(far, block, other), jnp.where(far, other, block)], axis=1)
    over = swap(pair, axis, 1)
    first, second = jnp.where(near, pair, over), jnp.where(near, over, pair)
    return jnp.concatenate(
        [first[:, :width], second[:, :width], first[:, width:], second[:, width:]], axis=1
    )


def near_sums(partial, axis):
    index = lax.axis_index(axis)
    far, near = index // 2 == 0, index % 2 == 0
    a, b, c, d = jnp.split(partial, 4, axis=1)
    give = jnp.concatenate([jnp.where(near, b, a), jnp.where(near, d, c)], axis=1)
    keep = jnp.concatenate([jnp.where(near, a, b), jnp.where(near, c, d)], axis=1)
    keep = keep + swap(give.astype(jnp.bfloat16), axis, 1).astype(jnp.float32)
    low, high = jnp.split(keep, 2, axis=1)
    return jnp.where(far, low, high), jnp.where(far, high, low).astype(jnp.bfloat16)


def feature_blocks(block):
    long, wide = lax.axis_size("sp"), lax.axis_size("tp")
    share = block.shape[1] // long
    me, mine = lax.axis_index("sp"), lax.axis_index("tp")
    if long != 2 * wide or wide != 4:
        sent = [block[:, s * share : (s + 1) * share] for s in range(long)]
        if small("sp"):
            sent = [
                lax.dynamic_slice_in_dim(block, (me ^ s) * share, share, 1) for s in range(long)
            ]
        numbers = [me ^ s if small("sp") else s for s in range(long)]
        return exchange(sent, "sp"), numbers
    pieces, numbers = [], []
    for turn in (0, 1):
        half = me // wide ^ turn
        sent = lax.dynamic_slice_in_dim(block, (2 * mine + half) * share, share, 1)
        route = [
            (i * wide + j, (2 * j + (i // wide ^ turn)) * wide + i % wide)
            for i in range(long)
            for j in range(wide)
        ]
        pieces.append(lax.ppermute(sent, ("sp", "tp"), route))
        numbers.append(wide * (me % 2 ^ turn))
    pair = jnp.concatenate(pieces, axis=0)
    far = swap(pair, "tp", 2)
    over = swap(jnp.concatenate([pair, far], axis=0), "tp", 1)
    return [pair, far, over], [n + (mine ^ m) for m in (0, 2, 1, 3) for n in numbers]


def gather_small(value, axis):
    if small(axis):
        return [value] + [swap(value, axis, s) for s in range(1, lax.axis_size(axis))]
    moved = lax.all_gather(value, axis, axis=0)
    return [moved[s] for s in range(lax.axis_size(axis))]


def shifted(block, axis, distance):
    devices = range(lax.axis_size(axis))
    route = [(i - distance, i) for i in devices if i - distance in devices]
    return lax.ppermute(block, axis, route)


def silu_slope(value, sigma):
    return sigma * (1.0 + value * (1.0 - sigma))


def contract_last(left, right):
    return lax.dot_general(
        left, right, (((1,), (1,)), ((), ())), preferred_element_type=jnp.float32
    )


def contract_first(left, right):
    return lax.dot_general(
        left, right, (((0,), (0,)), ((), ())), preferred_element_type=jnp.float32
    )


def body(
    stream,
    upstream,
    expert_gain,
    expert_ids,
    group_weight,
    pair_scores,
    gate_weight,
    up_weight,
    down_weight,
    mixer_weight,
    filtered,
    channel_gain,
    kernel_taps,
    value_branch,
    gate_branch,
):
    experts = lax.axis_size("sp")
    tokens_here, width = stream.shape
    capacity = max(2, 5 * tokens_here // (2 * experts))
    room = -(-capacity // 8) * 8
    groups = lax.axis_size("tp")
    column = width // groups
    first_col = lax.axis_index("tp") * column
    bf16 = jnp.bfloat16

    ids = expert_ids.T
    block_of = ids ^ lax.axis_index("sp") if small("sp") else ids
    lanes = jnp.arange(experts, dtype=jnp.int32)
    named = [(block_of[k][None, :] == lanes[:, None]).astype(jnp.float32) for k in (0, 1)]
    both = (named[0] + named[1]).astype(bf16)
    order = jnp.arange(tokens_here, dtype=jnp.int32)
    earlier = (order[:, None] < order[None, :]).astype(bf16)
    before = jnp.dot(both, earlier, preferred_element_type=jnp.float32)
    slots = [
        block_of[k] * room + jnp.sum(before * named[k], axis=0).astype(jnp.int32) for k in (0, 1)
    ]
    places = jnp.arange(experts * room, dtype=jnp.int32)
    hit0 = places[:, None] == slots[0][None, :]
    hit1 = places[:, None] == slots[1][None, :]
    pick = (hit0 | hit1).astype(bf16)
    spread = pair_scores[:, 0] - pair_scores[:, 1]
    weight0 = group_weight * jax.nn.sigmoid(spread)
    weight1 = group_weight * jax.nn.sigmoid(-spread)
    slot_weight = jnp.sum(
        jnp.where(hit0, weight0[None, :], 0.0) + jnp.where(hit1, weight1[None, :], 0.0), axis=1
    )

    stream_f = stream.astype(jnp.float32)
    inv_rms = lax.rsqrt(jnp.mean(stream_f * stream_f, axis=1, keepdims=True) + EPS)
    stream_part = lax.dynamic_slice_in_dim(stream, first_col, column, 1).astype(jnp.float32)
    gain_part = lax.dynamic_slice_in_dim(expert_gain, first_col, column, 0)
    upstream_part = lax.dynamic_slice_in_dim(upstream, first_col, column, 1)
    normed_part = (stream_part * inv_rms * gain_part).astype(bf16)
    send_rows = jnp.dot(pick, normed_part, preferred_element_type=jnp.float32).astype(bf16)
    send_cots = (
        slot_weight[:, None] * jnp.dot(pick, upstream_part, preferred_element_type=jnp.float32)
    ).astype(bf16)

    def block_list(array):
        return [array[s * room : (s + 1) * room] for s in range(experts)]

    got_rows = jnp.concatenate(exchange(block_list(send_rows), "sp"), axis=0)
    cot_blocks = block_list(send_cots)
    if small("sp"):
        early = -(-5 * experts // 8)
        first = [cot_blocks[0]] + [swap(cot_blocks[s], "sp", s) for s in range(1, early)]
        got_rows, late = lax.optimization_barrier((got_rows, cot_blocks[early:]))
        got_cots = first + [swap(b, "sp", s) for s, b in enumerate(late, early)]
    else:
        got_cots = exchange(cot_blocks, "sp")
    got_cots = jnp.concatenate(got_cots, axis=0)

    filt = filtered.astype(jnp.float32)
    here = filt.shape[1]
    channels = here * groups
    own_mean = jnp.mean(filt, axis=1)
    own_square = jnp.sum((filt - own_mean[:, None]) ** 2, axis=1)
    stats = gather_small(jnp.stack([own_mean, own_square]), "tp")
    stats, got_rows = lax.optimization_barrier((stats, got_rows))
    rows = gather_columns(got_rows, "tp")
    mean_c = sum(part[0] for part in stats) / groups
    squares = sum(part[1] + here * (part[0] - mean_c) ** 2 for part in stats)
    inv_std = lax.rsqrt(squares / channels + EPS)[:, None]
    centred = (filt - mean_c[:, None]) * inv_std
    normal_out = centred * channel_gain
    sig_norm = jax.nn.sigmoid(normal_out)
    activated = (normal_out * sig_norm).astype(bf16)
    slope = silu_slope(normal_out, sig_norm) * channel_gain
    activated, got_cots = lax.optimization_barrier((activated, got_cots))
    cots = gather_columns(got_cots, "tp")
    all_activated = gather_tokens(activated, "sp")

    gate_local = gate_weight[0]
    up_local = up_weight[0]
    down_local = down_weight[0]
    pre_gate = jnp.dot(rows, gate_local, preferred_element_type=jnp.float32)
    pre_up = jnp.dot(rows, up_local, preferred_element_type=jnp.float32)
    sigma = jax.nn.sigmoid(pre_gate)
    silu_gate = pre_gate * sigma
    hidden = (silu_gate * pre_up).astype(bf16)
    grad_hidden = contract_last(cots, down_local)
    grad_pre_gate = (grad_hidden * pre_up * silu_slope(pre_gate, sigma)).astype(bf16)
    grad_pre_up = (grad_hidden * silu_gate).astype(bf16)
    grad_pre_gate, grad_pre_up, all_activated = lax.optimization_barrier(
        (grad_pre_gate, grad_pre_up, all_activated)
    )
    partial_rows = contract_last(grad_pre_gate, gate_local) + contract_last(grad_pre_up, up_local)
    if groups == 4:
        own, give = near_sums(partial_rows, "tp")
        give, rows, cots, hidden, grad_pre_gate, grad_pre_up = lax.optimization_barrier(
            (give, rows, cots, hidden, grad_pre_gate, grad_pre_up)
        )
        shared = (own + swap(give, "tp", 2).astype(jnp.float32)).astype(bf16)
    else:
        shared = lax.psum_scatter(
            partial_rows.astype(bf16), "tp", scatter_dimension=1, tiled=True
        )
    gradient_gate = contract_first(rows, grad_pre_gate)[None]
    gradient_up = contract_first(rows, grad_pre_up)[None]
    gradient_down = contract_first(hidden, cots)[None]
    shared, gradient_gate, gradient_up, gradient_down = lax.optimization_barrier(
        (shared, gradient_gate, gradient_up, gradient_down)
    )
    back = jnp.concatenate(exchange(block_list(shared), "sp"), axis=0)

    grad_part = contract_first(pick, back).astype(bf16)
    grad_normed = gather_columns(grad_part, "tp").astype(jnp.float32)
    weighted = grad_normed * expert_gain
    inner = jnp.mean(weighted * stream_f, axis=1, keepdims=True)
    grad_stream = (
        upstream.astype(jnp.float32)
        + inv_rms * weighted
        - stream_f * inv_rms * inv_rms * inv_rms * inner
    ).astype(bf16)
    grad_blocks, numbers = feature_blocks(grad_stream)
    all_activated = all_activated.reshape(experts, tokens_here, -1)
    if small("sp"):
        numbers = [lax.axis_index("sp") ^ n for n in numbers]
    matching = jnp.concatenate(
        [lax.dynamic_index_in_dim(all_activated, n, 0, keepdims=False) for n in numbers], axis=0
    )
    gradient_mixer = contract_first(jnp.concatenate(grad_blocks, axis=0), matching)

    grad_act = contract_last(grad_stream, mixer_weight)
    grad_centred = grad_act * slope
    sums = gather_small(
        jnp.stack([jnp.sum(grad_centred, axis=1), jnp.sum(grad_centred * centred, axis=1)]), "tp"
    )
    slope_sum, slope_cross = sum(sums[1:], sums[0]) / channels
    grad_filtered = (
        inv_std * (grad_centred - slope_sum[:, None] - centred * slope_cross[:, None])
    ).astype(bf16)
    reach = kernel_taps.shape[0] - 1
    ahead = shifted(grad_filtered[:reach], "sp", -1)
    extended = jnp.concatenate([grad_filtered, ahead], axis=0).astype(jnp.float32)
    grad_mixed = lax.conv_general_dilated(
        extended[None],
        kernel_taps[::-1][:, None, :],
        (1,),
        "VALID",
        dimension_numbers=("NWC", "WIO", "NWC"),
        feature_group_count=here,
        precision=lax.Precision.HIGHEST,
    )[0]
    sig_gate = jax.nn.sigmoid(gate_branch.astype(jnp.float32))
    gradient_value = (grad_mixed * sig_gate).astype(bf16)
    gradient_gating = (
        grad_mixed * value_branch.astype(jnp.float32) * sig_gate * (1.0 - sig_gate)
    ).astype(bf16)
    return (
        gradient_value,
        gradient_gating,
        gradient_mixer,
        gradient_gate,
        gradient_up,
        gradient_down,
    )


def solution(mesh):
    return jax.shard_map(
        body,
        mesh=mesh,
        in_specs=(
            P("sp", None),
            P("sp", None),
            P(),
            P("sp", None),
            P("sp"),
            P("sp", None),
            P("sp", None, "tp"),
            P("sp", None, "tp"),
            P("sp", "tp", None),
            P("tp", None),
            P("sp", "tp"),
            P("tp"),
            P(None, "tp"),
            P("sp", "tp"),
            P("sp", "tp"),
        ),
        out_specs=(
            P("sp", "tp"),
            P("sp", "tp"),
            P("sp", "tp"),
            P("sp", None, "tp"),
            P("sp", None, "tp"),
            P("sp", "tp", None),
        ),
        check_vma=False,
    )
```

```python
import jax
import jax.numpy as jnp
from jax import lax
from jax.sharding import PartitionSpec as P

EPS = 1e-06


def swap(block, axis, mask):
    return lax.ppermute(block, axis, [(i, i ^ mask) for i in range(lax.axis_size(axis))])


def small(axis):
    size = lax.axis_size(axis)
    return size <= 8 and size & (size - 1) == 0


def exchange(blocks, axis):
    if small(axis):
        return [blocks[0]] + [swap(blocks[s], axis, s) for s in range(1, len(blocks))]
    moved = lax.all_to_all(jnp.stack(blocks), axis, split_axis=0, concat_axis=0, tiled=True)
    return [moved[s] for s in range(len(blocks))]


def gather_even(block, axis):
    if not small(axis) or lax.axis_size(axis) < 2:
        return block
    return jnp.stack([block] + [swap(block, axis, s) for s in range(2, lax.axis_size(axis), 2)])


def gather_odd(even, axis):
    if not small(axis) or lax.axis_size(axis) < 2:
        return lax.all_gather(even, axis, axis=0, tiled=True)
    return swap(even, axis, 1)


def gather_columns(block, axis):
    if lax.axis_size(axis) != 4:
        return lax.all_gather(block, axis, axis=1, tiled=True)
    index = lax.axis_index(axis)
    far, near = index // 2 == 0, index % 2 == 0
    other = swap(block, axis, 2)
    width = block.shape[1]
    pair = jnp.concatenate([jnp.where(far, block, other), jnp.where(far, other, block)], axis=1)
    over = swap(pair, axis, 1)
    first, second = jnp.where(near, pair, over), jnp.where(near, over, pair)
    return jnp.concatenate(
        [first[:, :width], second[:, :width], first[:, width:], second[:, width:]], axis=1
    )


def near_sums(partial, axis):
    index = lax.axis_index(axis)
    far, near = index // 2 == 0, index % 2 == 0
    a, b, c, d = jnp.split(partial, 4, axis=1)
    give = jnp.concatenate([jnp.where(near, b, a), jnp.where(near, d, c)], axis=1)
    keep = jnp.concatenate([jnp.where(near, a, b), jnp.where(near, c, d)], axis=1)
    keep = keep + swap(give.astype(jnp.bfloat16), axis, 1).astype(jnp.float32)
    low, high = jnp.split(keep, 2, axis=1)
    return jnp.where(far, low, high), jnp.where(far, high, low).astype(jnp.bfloat16)


def gather_small(value, axis):
    if small(axis):
        return [value] + [swap(value, axis, s) for s in range(1, lax.axis_size(axis))]
    moved = lax.all_gather(value, axis, axis=0)
    return [moved[s] for s in range(lax.axis_size(axis))]


def shifted(block, axis, distance):
    devices = range(lax.axis_size(axis))
    route = [(i - distance, i) for i in devices if i - distance in devices]
    return lax.ppermute(block, axis, route)


def silu_slope(value, sigma):
    return sigma * (1.0 + value * (1.0 - sigma))


def contract_last(left, right):
    return lax.dot_general(
        left, right, (((1,), (1,)), ((), ())), preferred_element_type=jnp.float32
    )


def contract_first(left, right):
    return lax.dot_general(
        left, right, (((0,), (0,)), ((), ())), preferred_element_type=jnp.float32
    )


def body(
    stream,
    upstream,
    expert_gain,
    expert_ids,
    group_weight,
    pair_scores,
    gate_weight,
    up_weight,
    down_weight,
    mixer_weight,
    filtered,
    channel_gain,
    kernel_taps,
    value_branch,
    gate_branch,
):
    experts = lax.axis_size("sp")
    tokens_here, width = stream.shape
    capacity = max(2, 5 * tokens_here // (2 * experts))
    room = -(-capacity // 8) * 8
    groups = lax.axis_size("tp")
    column = width // groups
    first_col = lax.axis_index("tp") * column
    bf16 = jnp.bfloat16

    ids = expert_ids.T
    block_of = ids ^ lax.axis_index("sp") if small("sp") else ids
    lanes = jnp.arange(experts, dtype=jnp.int32)
    named = [(block_of[k][None, :] == lanes[:, None]).astype(jnp.float32) for k in (0, 1)]
    both = (named[0] + named[1]).astype(bf16)
    order = jnp.arange(tokens_here, dtype=jnp.int32)
    earlier = (order[:, None] < order[None, :]).astype(bf16)
    before = jnp.dot(both, earlier, preferred_element_type=jnp.float32)
    slots = [
        block_of[k] * room + jnp.sum(before * named[k], axis=0).astype(jnp.int32) for k in (0, 1)
    ]
    places = jnp.arange(experts * room, dtype=jnp.int32)
    hit0 = places[:, None] == slots[0][None, :]
    hit1 = places[:, None] == slots[1][None, :]
    pick = (hit0 | hit1).astype(bf16)
    spread = pair_scores[:, 0] - pair_scores[:, 1]
    weight0 = group_weight * jax.nn.sigmoid(spread)
    weight1 = group_weight * jax.nn.sigmoid(-spread)
    slot_weight = jnp.sum(
        jnp.where(hit0, weight0[None, :], 0.0) + jnp.where(hit1, weight1[None, :], 0.0), axis=1
    )

    stream_f = stream.astype(jnp.float32)
    inv_rms = lax.rsqrt(jnp.mean(stream_f * stream_f, axis=1, keepdims=True) + EPS)
    stream_part = lax.dynamic_slice_in_dim(stream, first_col, column, 1).astype(jnp.float32)
    gain_part = lax.dynamic_slice_in_dim(expert_gain, first_col, column, 0)
    upstream_part = lax.dynamic_slice_in_dim(upstream, first_col, column, 1)
    normed_part = (stream_part * inv_rms * gain_part).astype(bf16)
    send_rows = jnp.dot(pick, normed_part, preferred_element_type=jnp.float32).astype(bf16)
    send_cots = (
        slot_weight[:, None] * jnp.dot(pick, upstream_part, preferred_element_type=jnp.float32)
    ).astype(bf16)

    def block_list(array):
        return [array[s * room : (s + 1) * room] for s in range(experts)]

    got_rows = jnp.concatenate(exchange(block_list(send_rows), "sp"), axis=0)
    got_cots = jnp.concatenate(exchange(block_list(send_cots), "sp"), axis=0)

    filt = filtered.astype(jnp.float32)
    here = filt.shape[1]
    channels = here * groups
    own_mean = jnp.mean(filt, axis=1)
    own_square = jnp.sum((filt - own_mean[:, None]) ** 2, axis=1)
    own_stats, got_rows = lax.optimization_barrier(
        (jnp.stack([own_mean, own_square]), got_rows)
    )
    rows = gather_columns(got_rows, "tp")
    cots = gather_columns(got_cots, "tp")
    stats = gather_small(own_stats, "tp")
    mean_c = sum(part[0] for part in stats) / groups
    squares = sum(part[1] + here * (part[0] - mean_c) ** 2 for part in stats)
    inv_std = lax.rsqrt(squares / channels + EPS)[:, None]
    centred = (filt - mean_c[:, None]) * inv_std
    normal_out = centred * channel_gain
    sig_norm = jax.nn.sigmoid(normal_out)
    activated = (normal_out * sig_norm).astype(bf16)
    slope = silu_slope(normal_out, sig_norm) * channel_gain

    gate_local = gate_weight[0]
    up_local = up_weight[0]
    down_local = down_weight[0]
    pre_gate = jnp.dot(rows, gate_local, preferred_element_type=jnp.float32)
    pre_up = jnp.dot(rows, up_local, preferred_element_type=jnp.float32)
    sigma = jax.nn.sigmoid(pre_gate)
    silu_gate = pre_gate * sigma
    hidden = (silu_gate * pre_up).astype(bf16)
    grad_hidden = contract_last(cots, down_local)
    grad_pre_gate = (grad_hidden * pre_up * silu_slope(pre_gate, sigma)).astype(bf16)
    grad_pre_up = (grad_hidden * silu_gate).astype(bf16)
    partial_rows = contract_last(grad_pre_gate, gate_local) + contract_last(grad_pre_up, up_local)
    if groups == 4:
        own, give = near_sums(partial_rows, "tp")
        give, activated, hidden, grad_pre_gate, grad_pre_up = lax.optimization_barrier(
            (give, activated, hidden, grad_pre_gate, grad_pre_up)
        )
        shared = (own + swap(give, "tp", 2).astype(jnp.float32)).astype(bf16)
    else:
        shared = lax.psum_scatter(
            partial_rows.astype(bf16), "tp", scatter_dimension=1, tiled=True
        )
    even = gather_even(activated, "sp")
    gradient_gate = contract_first(rows, grad_pre_gate)[None]
    gradient_up = contract_first(rows, grad_pre_up)[None]
    gradient_down = contract_first(hidden, cots)[None]
    shared, even, gradient_gate, gradient_up, gradient_down = lax.optimization_barrier(
        (shared, even, gradient_gate, gradient_up, gradient_down)
    )
    back = jnp.concatenate(exchange(block_list(shared), "sp"), axis=0)
    odd = gather_odd(even, "sp")
    back, odd = lax.optimization_barrier((back, odd))
    if even.ndim == 3:
        all_activated = jnp.stack([even, odd], axis=1).reshape(experts * tokens_here, -1)
    else:
        all_activated = odd

    grad_part = contract_first(pick, back).astype(bf16)
    grad_normed = gather_columns(grad_part, "tp").astype(jnp.float32)
    weighted = grad_normed * expert_gain
    inner = jnp.mean(weighted * stream_f, axis=1, keepdims=True)
    grad_stream = (
        upstream.astype(jnp.float32)
        + inv_rms * weighted
        - stream_f * inv_rms * inv_rms * inv_rms * inner
    ).astype(bf16)
    share = width // experts
    sent = [grad_stream[:, s * share : (s + 1) * share] for s in range(experts)]
    if small("sp"):
        me = lax.axis_index("sp")
        sent = [
            lax.dynamic_slice_in_dim(grad_stream, (me ^ s) * share, share, 1)
            for s in range(experts)
        ]
    all_grads = jnp.concatenate(exchange(sent, "sp"), axis=0)
    gradient_mixer = contract_first(all_grads, all_activated)

    grad_act = contract_last(grad_stream, mixer_weight)
    grad_centred = grad_act * slope
    sums = gather_small(
        jnp.stack([jnp.sum(grad_centred, axis=1), jnp.sum(grad_centred * centred, axis=1)]), "tp"
    )
    slope_sum, slope_cross = sum(sums[1:], sums[0]) / channels
    grad_filtered = (
        inv_std * (grad_centred - slope_sum[:, None] - centred * slope_cross[:, None])
    ).astype(bf16)
    reach = kernel_taps.shape[0] - 1
    ahead = shifted(grad_filtered[:reach], "sp", -1)
    extended = jnp.concatenate([grad_filtered, ahead], axis=0).astype(jnp.float32)
    grad_mixed = lax.conv_general_dilated(
        extended[None],
        kernel_taps[::-1][:, None, :],
        (1,),
        "VALID",
        dimension_numbers=("NWC", "WIO", "NWC"),
        feature_group_count=here,
        precision=lax.Precision.HIGHEST,
    )[0]
    sig_gate = jax.nn.sigmoid(gate_branch.astype(jnp.float32))
    gradient_value = (grad_mixed * sig_gate).astype(bf16)
    gradient_gating = (
        grad_mixed * value_branch.astype(jnp.float32) * sig_gate * (1.0 - sig_gate)
    ).astype(bf16)
    return (
        gradient_value,
        gradient_gating,
        gradient_mixer,
        gradient_gate,
        gradient_up,
        gradient_down,
    )


def solution(mesh):
    return jax.shard_map(
        body,
        mesh=mesh,
        in_specs=(
            P("sp", None),
            P("sp", None),
            P(),
            P("sp", None),
            P("sp"),
            P("sp", None),
            P("sp", None, "tp"),
            P("sp", None, "tp"),
            P("sp", "tp", None),
            P("tp", None),
            P("sp", "tp"),
            P("tp"),
            P(None, "tp"),
            P("sp", "tp"),
            P("sp", "tp"),
        ),
        out_specs=(
            P("sp", "tp"),
            P("sp", "tp"),
            P("sp", "tp"),
            P("sp", None, "tp"),
            P("sp", None, "tp"),
            P("sp", "tp", None),
        ),
        check_vma=False,
    )
```
